32 devices in a mesh: sp: 8 (over z, x), tp: 4 (over y, core).
Axes of the slice: x: 2, y: 2, z: 4, core: 2. Of those that a mesh axis runs over, the one named last changes fastest.
Arguments:
- residual: bfloat16 [1536, 2048], P('sp', 'tp'), may hold values from -10 to 10
- queries: bfloat16 [1536, 16, 128], P('sp', 'tp'), may hold values from -6.5 to 6.5
- key_rows: bfloat16 [1536, 16, 128], P('sp', 'tp'), may hold values from -6.5 to 6.5
- value_rows: bfloat16 [1536, 16, 128], P('sp', 'tp'), may hold values from -6 to 6
- diff_scale: float32 [16], P('tp'), may hold values from 0.3 to 0.8
- head_gain: float32 [128], replicated, may hold values from 0.1 to 1.9
- out_weight: bfloat16 [2048, 2048], P(None, 'tp'), may hold values from -0.125 to 0.125
- norm_gain: float32 [2048], replicated, may hold values from 0.1 to 1.9
- gate_weight: bfloat16 [8, 2048, 4096], P('sp', None, 'tp'), may hold values from -0.5 to 0.5
- up_weight: bfloat16 [8, 2048, 4096], P('sp', None, 'tp'), may hold values from -0.5 to 0.5
- down_weight: bfloat16 [8, 4096, 2048], P('sp', None, 'tp'), may hold values from -0.01171875 to 0.01171875
- expert_ids: int32 [1536, 2], P('sp'), may hold values from 0 to 7, all different within a row; in each aligned block of 192 rows (0 to 191, 192 to 383, ...) at most 96 rows name the same one
- route_logit: float32 [1536, 2], P('sp'), may hold values from -6 to 6
Outputs:
- updated: bfloat16 [1536, 2048], P('sp', 'tp')
The draws below stay inside these ranges and needn't reach their ends.
Inputs may be any that keep to these rules, and one draw needn't show every extreme that they name: `expert_ids`: A token's 2 experts differ. The 192 tokens of one index of sp name one expert at most 96 times, a bound that some block reaches on some index.
All inputs are finite; a program needn't handle non-finite values.
Results may differ from the reference program's by a relative error of at most 0.014.
Values may be sent and summed in bfloat16 or wider, within the bound.
A program may use at most 64 MiB of HBM per device.

```python
import math
import jax
import jax.numpy as jnp
import numpy as np
from jax import lax

D = 2048
HEADS = 16
QK = 64
V = 128
FF = 4096
TOP = 2
SPAN = 64
TOK_DEV = 192
TOKENS = 1536
EXPERTS = 8
CAP = 96
N_SP = 8


def drawn_pair(base):
    folded_key = jax.random.fold_in(base, 17)
    keys_list = jax.random.split(folded_key, 2)
    array_shape = (TOKENS, HEADS, 2 * QK)
    query_values = jnp.clip(1.3 * jax.random.normal(keys_list[0], array_shape, jnp.float32), -6.5, 6.5)
    key_values = jnp.clip(1.3 * jax.random.normal(keys_list[1], array_shape, jnp.float32), -6.5, 6.5)
    return (query_values, key_values)


def draw_queries(key, part):
    return drawn_pair(key)[0].astype(jnp.bfloat16)


def draw_key_rows(key, part):
    return drawn_pair(key)[1].astype(jnp.bfloat16)


def draw_residual(key, part):
    first = jax.random.fold_in(jax.random.fold_in(key, 29), 0)
    column = jnp.arange(D, dtype=jnp.float32) / D
    values = jnp.clip(jax.random.normal(first, (TOKENS, D), jnp.float32), -6.0, 6.0) * 0.5 * 3.0 ** column
    return values.astype(jnp.bfloat16)


def steps_of(rng, dims, cuts, least, top_value):
    factor_of, own = 1.0, jax.random.fold_in(rng, 6)
    for position, shards_of in cuts:
        steps = jnp.exp(jax.random.uniform(jax.random.fold_in(own, position), (shards_of,), jnp.float32, least / len(cuts), top_value / len(cuts)))
        factor_of = factor_of * jnp.repeat(steps, dims[position] // shards_of).reshape([-1 if axis == position else 1 for axis in range(len(dims))])
    return factor_of


def assign_block(rng, own, number, rows, number_of, top, limit, slope):
    sequence = jax.random.permutation(rng, number_of)
    packed, usual = portions_of(number_of, rows * top, limit, slope, True), portions_of(number_of, rows * top, limit, slope, False)
    places = jnp.arange(number_of)

    def named(tallies, offset_by):
        used = int((tallies > 0).sum())
        fixed = max(1, used // 4)
        passed = fixed + (places - fixed + offset_by * (used - fixed)) % max(1, number_of - fixed)
        return jnp.zeros((number_of,), jnp.int32).at[sequence[jnp.where(places < fixed, places, passed)]].set(jnp.asarray(tallies, jnp.int32))

    tallies = jnp.where(number % 4 == 0, named(packed, number // 4), named(usual, number - number // 4 - 1))
    mixed = jax.random.permutation(jax.random.fold_in(own, 3), number_of)
    donor, taker = mixed[0:number_of // 2 * 2:2], mixed[1:number_of // 2 * 2:2]
    margin = jnp.minimum(tallies[donor] - 1, limit - tallies[taker]) // 2
    margin = jnp.where((donor == sequence[0]) | (taker == sequence[0]) | (tallies[taker] == 0), 0, jnp.maximum(margin, 0))
    passed = jax.random.randint(jax.random.fold_in(own, 4), (number_of // 2,), 0, 1 << 20) % (margin + 1)
    tallies = tallies.at[donor].add(-passed).at[taker].add(passed)
    items = jnp.searchsorted(jnp.cumsum(tallies), jnp.arange(rows * top), side="right").astype(jnp.int32)
    listing = items.reshape(top, rows).T
    listing = listing[jax.random.permutation(jax.random.fold_in(own, 1), rows)]
    offset_by = jax.random.randint(jax.random.fold_in(own, 2), (rows, 1), 0, top)
    return jnp.take_along_axis(listing, (jnp.arange(top)[None, :] + offset_by) % top, axis=1)


def portions_of(number_of, total, reach, skew, full):
    portions = [(1 << 20) // math.isqrt(grade ** skew) + 1 for grade in range(1, number_of + 1)]
    largest = reach if full else min(reach, max(-(-total // number_of), total * portions[0] // sum(portions)))
    least = 1 if total - largest >= number_of - 1 else 0
    counts, rest = [largest] + [least] * (number_of - 1), total - largest - least * (number_of - 1)
    while rest > 0:
        free = [i for i in range(1, number_of) if counts[i] < largest] or [i for i in range(1, number_of) if counts[i] < reach]
        pool, remaining = sum([portions[i] for i in free]), rest
        for i in free:
            more = min(reach - counts[i], max(1, remaining * portions[i] // pool), rest)
            counts[i] = counts[i] + more
            rest = rest - more
    return np.array(counts)


def centred(own_key, extent, deviation, most, pieces=(), held_as=jnp.bfloat16):
    values = deviation * jax.random.normal(own_key, extent, jnp.float32)
    if pieces:
        values = values * steps_of(own_key, extent, pieces, -0.22, 0.18)
    return jnp.clip(values, -most, most).astype(held_as)


def setup_inputs(seed: int = 0) -> dict:
    keys = jax.random.split(jax.random.key(seed), 14)
    residual = draw_residual(jax.random.fold_in(keys[13], 71), 0)
    queries = draw_queries(jax.random.fold_in(keys[13], 71), 0)
    key_rows = draw_key_rows(jax.random.fold_in(keys[13], 71), 0)
    value_rows = centred(keys[3], (TOKENS, HEADS, V), 1.0, 6.0, ((0, 8), (1, 4)))
    diff_scale = jnp.clip(0.3 + 0.5 * jax.random.uniform(keys[4], (HEADS,), jnp.float32) ** steps_of(keys[4], (HEADS,), ((0, 4),), -0.2, 0.2), 0.3, 0.8)
    head_gain = jnp.clip(1.0 + 0.18 * jax.random.normal(keys[5], (V,), jnp.float32), 0.1, 1.9)
    out_weight = centred(keys[6], (HEADS * V, D), (HEADS * V) ** -0.5, 0.125, ((1, 4),))
    norm_gain = jnp.clip(1.0 + 0.18 * jax.random.normal(keys[7], (D,), jnp.float32), 0.1, 1.9)
    gate_weight = centred(keys[8], (EXPERTS, D, FF), (D // 16) ** -0.5, 0.5, ((0, 8), (2, 4)))
    up_weight = centred(keys[9], (EXPERTS, D, FF), (D // 16) ** -0.5, 0.5, ((0, 8), (2, 4)))
    down_weight = centred(keys[10], (EXPERTS, FF, D), (FF * 64) ** -0.5, 0.01171875, ((0, 8), (2, 4)))
    expert_ids_keys = jax.random.split(jax.random.fold_in(keys[11], 1), TOKENS // TOK_DEV)
    expert_ids_turns = jax.random.permutation(jax.random.fold_in(keys[11], 3), TOKENS // TOK_DEV)
    expert_ids = jax.vmap(lambda own, number: assign_block(jax.random.fold_in(keys[11], 2), own, number, TOK_DEV, EXPERTS, TOP, CAP, 2))(expert_ids_keys, expert_ids_turns).reshape((TOKENS, TOP))
    route_logit = centred(keys[12], (TOKENS, TOP), 1.5, 6.0, ((0, 8),), jnp.float32)
    return {"residual": residual, "queries": queries, "key_rows": key_rows, "value_rows": value_rows, "diff_scale": diff_scale, "head_gain": head_gain, "out_weight": out_weight, "norm_gain": norm_gain, "gate_weight": gate_weight, "up_weight": up_weight, "down_weight": down_weight, "expert_ids": expert_ids, "route_logit": route_logit}


NORM_EPS = 1e-05
CLAMP_LIMIT = 7.0
SWISH_ALPHA = 1.702
HEAD_KEEP = 0.8

def one_map(query_half, key_half, value_all, visible):
    scores = jnp.einsum('qhd,khd->hqk', query_half, key_half) * QK ** (-0.5)
    scores = jnp.where(visible[None], scores, -jnp.inf)
    row_peak = lax.optimization_barrier(jnp.max(scores, axis=-1, keepdims=True))
    exp_weights = jnp.where(visible[None], jnp.exp(scores - row_peak), 0.0)
    row_total = lax.optimization_barrier(jnp.sum(exp_weights, axis=-1))
    rounded = lax.optimization_barrier(exp_weights.astype(jnp.bfloat16)).astype(jnp.float32)
    accum = jnp.einsum('hqk,khv->hqv', rounded, value_all)
    return accum / row_total[..., None]

def reference(residual, queries, key_rows, value_rows, diff_scale, head_gain, out_weight, norm_gain, gate_weight, up_weight, down_weight, expert_ids, route_logit):
    block_rows = math.gcd(TOKENS, 512)
    key_all = key_rows.astype(jnp.float32)
    value_all = value_rows.astype(jnp.float32)
    key_span = jnp.arange(TOKENS, dtype=jnp.int32) // SPAN

    def attend(block_index):
        first_row = (block_index * block_rows).astype(jnp.int32)
        query_block = lax.dynamic_slice_in_dim(queries, first_row, block_rows, 0).astype(jnp.float32)
        query_span = (first_row + jnp.arange(block_rows, dtype=jnp.int32)) // SPAN
        visible = key_span[None, :] <= query_span[:, None]
        first_map = one_map(query_block[..., :QK], key_all[..., :QK], value_all, visible)
        second_map = one_map(query_block[..., QK:], key_all[..., QK:], value_all, visible)
        mixture = first_map - diff_scale[:, None, None] * second_map
        scale_back = lax.rsqrt(lax.optimization_barrier(jnp.mean(mixture * mixture, axis=-1, keepdims=True)) + NORM_EPS)
        attended = (mixture * scale_back * head_gain * HEAD_KEEP).astype(jnp.bfloat16)
        return jnp.transpose(attended, (1, 0, 2)).reshape(block_rows, HEADS * V)
    attended = lax.map(attend, jnp.arange(TOKENS // block_rows, dtype=jnp.int32)).reshape(TOKENS, HEADS * V)
    projected = jnp.dot(attended, out_weight, preferred_element_type=jnp.float32)
    after_mixer = (residual.astype(jnp.float32) + projected).astype(jnp.bfloat16)
    mixer_float = after_mixer.astype(jnp.float32)
    square_total = lax.optimization_barrier(jnp.sum(mixer_float * mixer_float, axis=-1, keepdims=True))
    normed = (mixer_float * lax.rsqrt(square_total / D + NORM_EPS) * norm_gain).astype(jnp.bfloat16)
    chosen = expert_ids.reshape(N_SP, TOK_DEV * TOP)
    onehot = (chosen[..., None] == jnp.arange(EXPERTS, dtype=jnp.int32)).astype(jnp.int32)
    rank_in = (lax.optimization_barrier(jnp.sum(jnp.cumsum(onehot, axis=1).astype(jnp.int32) * onehot, axis=-1)) - 1).astype(jnp.int32)
    source = jnp.arange(N_SP, dtype=jnp.int32)[:, None]
    per_expert = N_SP * CAP
    slot_index = (chosen * per_expert + source * CAP + rank_in).reshape(TOKENS * TOP).astype(jnp.int32)
    token_of = jnp.arange(TOKENS * TOP, dtype=jnp.int32) // TOP
    owner_row = jnp.full((EXPERTS * per_expert,), TOKENS, jnp.int32).at[slot_index].set(token_of)
    padded = jnp.concatenate([normed, jnp.zeros((1, D), jnp.bfloat16)], axis=0)

    def run_expert(expert):
        rows_in = padded[lax.dynamic_slice_in_dim(owner_row, (expert * per_expert).astype(jnp.int32), per_expert, 0)]
        pre_gate = jnp.dot(rows_in, gate_weight[expert], preferred_element_type=jnp.float32)
        pre_up = jnp.dot(rows_in, up_weight[expert], preferred_element_type=jnp.float32)
        capped = jnp.minimum(pre_gate, CLAMP_LIMIT)
        linear = jnp.clip(pre_up, -CLAMP_LIMIT, CLAMP_LIMIT)
        hidden = (capped * jax.nn.sigmoid(SWISH_ALPHA * capped) * (linear + 1.0)).astype(jnp.bfloat16)
        return jnp.dot(hidden, down_weight[expert], preferred_element_type=jnp.float32).astype(jnp.bfloat16)
    expert_out = lax.map(run_expert, jnp.arange(EXPERTS, dtype=jnp.int32)).reshape(EXPERTS * per_expert, D)
    picked = expert_out[slot_index].astype(jnp.float32).reshape(TOKENS, TOP, D)
    weights = jax.nn.softmax(route_logit.astype(jnp.float32), axis=-1)
    routed = lax.optimization_barrier(jnp.sum(picked * weights[..., None], axis=1))
    return (mixer_float + routed).astype(jnp.bfloat16)
```

```python
import functools
import math

import jax
import jax.numpy as jnp
from jax import lax
from jax.experimental import pallas as pl
from jax.experimental.pallas import tpu as pltpu
from jax.sharding import PartitionSpec as P

D = 2048
QK = 64
SPAN = 64


NORM_EPS = 1e-05
CLAMP_LIMIT = 7.0
SWISH_ALPHA = 1.702
HEAD_KEEP = 0.8
NEG_FILL = -1e30


def update_map(running, query_half, key_half, value_block, visible):
    row_peak, row_total, accum = running
    scores = jnp.einsum(
        "qhd,khd->hqk", query_half, key_half, preferred_element_type=jnp.float32
    ) * QK ** (-0.5)
    scores = jnp.where(visible[None], scores, NEG_FILL)
    new_peak = jnp.maximum(row_peak, jnp.max(scores, axis=-1))
    exp_weights = jnp.where(visible[None], jnp.exp(scores - new_peak[..., None]), 0.0)
    rescale = jnp.exp(row_peak - new_peak)
    row_total = row_total * rescale + jnp.sum(exp_weights, axis=-1)
    accum = accum * rescale[..., None] + jnp.einsum(
        "hqk,khv->hqv",
        exp_weights.astype(jnp.bfloat16),
        value_block,
        preferred_element_type=jnp.float32,
    )
    return (new_peak, row_total, accum)


def expert_kernel(
    sp_size,
    tp_size,
    groups,
    outgoing,
    gate_hbm,
    up_hbm,
    down_hbm,
    returned,
    rows_in,
    hidden,
    result,
    gate,
    up,
    down,
    weight_sem,
    local_sem,
    disp_send,
    disp_recv,
    ret_send,
    ret_recv,
    row_send,
    row_recv,
    hid_send,
    hid_recv,
):
    me = lax.axis_index("sp")
    rank = lax.axis_index("tp")
    parity = lax.rem(rank, 2)
    sibling = rank + 1 - 2 * parity
    chips = tp_size // 2
    chip = rank // 2
    span = sp_size // groups
    cap = outgoing.shape[1]
    feats = outgoing.shape[2]
    units = gate.shape[1]
    columns = down.shape[1]

    weights = [
        pltpu.make_async_copy(src, dst, weight_sem.at[i])
        for i, (src, dst) in enumerate(((gate_hbm, gate), (up_hbm, up), (down_hbm, down)))
    ]
    for copy in weights:
        copy.start()

    def peer_rank(step):
        return lax.rem(chip + step, chips) * 2 + parity

    barrier = pltpu.get_barrier_semaphore()
    for step in range(1, sp_size):
        pl.semaphore_signal(
            barrier,
            inc=1,
            device_id={"sp": lax.rem(me + step, sp_size), "tp": rank},
            device_id_type=pl.DeviceIdType.MESH,
        )
    for step in range(1, chips):
        pl.semaphore_signal(
            barrier,
            inc=1,
            device_id={"sp": me, "tp": peer_rank(step)},
            device_id_type=pl.DeviceIdType.MESH,
        )
    pl.semaphore_signal(
        barrier,
        inc=1,
        device_id={"sp": me, "tp": sibling},
        device_id_type=pl.DeviceIdType.MESH,
    )
    pl.semaphore_wait(barrier, sp_size - 1 + chips)

    def slot(step):
        return rows_in.at[step // span, rank, pl.ds((step % span) * cap, cap)]

    def dispatch(step):
        expert = lax.rem(me + sp_size - step, sp_size)
        return pltpu.make_async_remote_copy(
            src_ref=outgoing.at[expert],
            dst_ref=slot(step),
            send_sem=disp_send.at[step],
            recv_sem=disp_recv.at[step],
            device_id={"sp": expert, "tp": rank},
            device_id_type=pl.DeviceIdType.MESH,
        )

    own_in = pltpu.make_async_copy(outgoing.at[me], slot(0), local_sem.at[0])
    own_in.start()
    for step in range(1, sp_size):
        dispatch(step).start()

    def piece(buffer, send, recv, group, owner, target, send_slot):
        return pltpu.make_async_remote_copy(
            src_ref=buffer.at[group, owner],
            dst_ref=buffer.at[group, owner],
            send_sem=send.at[group, send_slot],
            recv_sem=recv.at[group, owner],
            device_id={"sp": me, "tp": target},
            device_id_type=pl.DeviceIdType.MESH,
        )

    def spread(buffer, send, recv, group):
        for step in range(1, chips):
            target = peer_rank(step)
            piece(buffer, send, recv, group, rank, target, target).start()
        piece(buffer, send, recv, group, rank, sibling, sibling).start()

    def collect(buffer, send, recv, group):
        for step in range(1, chips):
            owner = peer_rank(step)
            forward = piece(buffer, send, recv, group, owner, sibling, owner + 1 - 2 * parity)
            forward.wait_recv()
            forward.start()
        for step in range(chips):
            owner = peer_rank(step) + 1 - 2 * parity
            piece(buffer, send, recv, group, owner, sibling, sibling).wait_recv()

    unit_tile = math.gcd(units, 256)
    column_tile = math.gcd(columns, 256)

    def spread_rows(group):
        for place in range(span):
            def arrived(place=place):
                step = group * span + place
                pltpu.make_async_remote_copy(
                    src_ref=outgoing.at[0],
                    dst_ref=rows_in.at[group, rank, pl.ds(place * cap, cap)],
                    send_sem=disp_send.at[step],
                    recv_sem=disp_recv.at[step],
                    device_id={"sp": me, "tp": sibling},
                    device_id_type=pl.DeviceIdType.MESH,
                ).wait_recv()

            if place == 0:
                @pl.when(group == 0)
                def _():
                    own_in.wait()

                pl.when(group > 0)(arrived)
            else:
                arrived()
        spread(rows_in, row_send, row_recv, group)

    def run_up(group):
        collect(rows_in, row_send, row_recv, group)

        @pl.when(group == 0)
        def _():
            weights[0].wait()
            weights[1].wait()

        @pl.loop(0, units // unit_tile)
        def _(tile):
            cols = pl.ds(pl.multiple_of(tile * unit_tile, unit_tile), unit_tile)
            pre_gate = 0.0
            pre_up = 0.0
            for part in range(tp_size):
                block = rows_in[group, part]
                depth = pl.ds(part * feats, feats)
                pre_gate += jnp.dot(block, gate[depth, cols], preferred_element_type=jnp.float32)
                pre_up += jnp.dot(block, up[depth, cols], preferred_element_type=jnp.float32)
            capped = jnp.minimum(pre_gate, CLAMP_LIMIT)
            linear = jnp.clip(pre_up, -CLAMP_LIMIT, CLAMP_LIMIT)
            value = capped * jax.nn.sigmoid(SWISH_ALPHA * capped) * (linear + 1.0)
            hidden[group, rank, :, cols] = value.astype(jnp.bfloat16)

        spread(hidden, hid_send, hid_recv, group)

    def give_back(step):
        source = lax.rem(me + step, sp_size)
        return pltpu.make_async_remote_copy(
            src_ref=result.at[step // span, pl.ds((step % span) * cap, cap)],
            dst_ref=returned.at[me],
            send_sem=ret_send.at[step],
            recv_sem=ret_recv.at[step],
            device_id={"sp": source, "tp": rank},
            device_id_type=pl.DeviceIdType.MESH,
        )

    own_out = pltpu.make_async_copy(result.at[0, pl.ds(0, cap)], returned.at[me], local_sem.at[1])

    def run_down(group):
        collect(hidden, hid_send, hid_recv, group)

        @pl.when(group == 0)
        def _():
            weights[2].wait()

        @pl.loop(0, columns // column_tile)
        def _(tile):
            cols = pl.ds(pl.multiple_of(tile * column_tile, column_tile), column_tile)
            total = 0.0
            for part in range(tp_size):
                total += jnp.dot(
                    hidden[group, part],
                    down[pl.ds(part * units, units), cols],
                    preferred_element_type=jnp.float32,
                )
            result[group, :, cols] = total.astype(jnp.bfloat16)

        for place in range(span):
            if place == 0:
                @pl.when(group == 0)
                def _():
                    own_out.start()

                @pl.when(group > 0)
                def _():
                    give_back(group * span).start()
            else:
                give_back(group * span + place).start()

    @pl.loop(0, groups + 2)
    def _(turn):
        @pl.when(turn < groups)
        def _():
            spread_rows(turn)

        @pl.when((turn >= 1) & (turn < groups + 1))
        def _():
            run_up(turn - 1)

        @pl.when(turn >= 2)
        def _():
            run_down(turn - 2)

    own_out.wait()
    for step in range(1, sp_size):
        dispatch(step).wait_send()
    for step in range(1, sp_size):
        back = give_back(step)
        back.wait_send()
        pltpu.make_async_remote_copy(
            src_ref=result.at[0, pl.ds(0, cap)],
            dst_ref=returned.at[lax.rem(me + sp_size - step, sp_size)],
            send_sem=ret_send.at[step],
            recv_sem=ret_recv.at[step],
            device_id={"sp": lax.rem(me + step, sp_size), "tp": rank},
            device_id_type=pl.DeviceIdType.MESH,
        ).wait_recv()

    @pl.loop(0, groups)
    def _(group):
        for buffer, send, recv in ((rows_in, row_send, row_recv), (hidden, hid_send, hid_recv)):
            for step in range(1, chips):
                target = peer_rank(step)
                piece(buffer, send, recv, group, rank, target, target).wait_send()
                other = target + 1 - 2 * parity
                piece(buffer, send, recv, group, target, sibling, other).wait_send()
            piece(buffer, send, recv, group, rank, sibling, sibling).wait_send()


def run_experts(outgoing, gate_weight, up_weight, down_weight):
    sp_size, cap, feats = outgoing.shape
    tp_size = lax.axis_size("tp")
    groups = math.gcd(sp_size, 4)
    rows = sp_size // groups * cap
    units = gate_weight.shape[1]
    columns = down_weight.shape[1]
    dma = pltpu.SemaphoreType.DMA
    return pl.pallas_call(
        functools.partial(expert_kernel, sp_size, tp_size, groups),
        out_shape=jax.ShapeDtypeStruct((sp_size, cap, columns), jnp.bfloat16),
        in_specs=[pl.BlockSpec(memory_space=pltpu.VMEM)]
        + [pl.BlockSpec(memory_space=pl.ANY)] * 3,
        out_specs=pl.BlockSpec(memory_space=pl.ANY),
        scratch_shapes=[
            pltpu.VMEM((groups, tp_size, rows, feats), jnp.bfloat16),
            pltpu.VMEM((groups, tp_size, rows, units), jnp.bfloat16),
            pltpu.VMEM((groups, rows, columns), jnp.bfloat16),
            pltpu.VMEM(gate_weight.shape, jnp.bfloat16),
            pltpu.VMEM(up_weight.shape, jnp.bfloat16),
            pltpu.VMEM(down_weight.shape, jnp.bfloat16),
            dma((3,)),
            dma((2,)),
            dma((sp_size,)),
            dma((sp_size,)),
            dma((sp_size,)),
            dma((sp_size,)),
            dma((groups, tp_size)),
            dma((groups, tp_size)),
            dma((groups, tp_size)),
            dma((groups, tp_size)),
        ],
        compiler_params=pltpu.CompilerParams(
            collective_id=0, has_side_effects=True, vmem_limit_bytes=48 * 1024 * 1024
        ),
    )(outgoing, gate_weight, up_weight, down_weight)


def local(
    residual,
    queries,
    key_rows,
    value_rows,
    diff_scale,
    head_gain,
    out_weight,
    norm_gain,
    gate_weight,
    up_weight,
    down_weight,
    expert_ids,
    route_logit,
):
    tokens_here = queries.shape[0]
    heads_here = queries.shape[1]
    value_width = value_rows.shape[2]
    query_start = lax.axis_index("sp") * tokens_here
    query_span = (query_start + jnp.arange(tokens_here, dtype=jnp.int32)) // SPAN
    first_query = queries[..., :QK]
    second_query = queries[..., QK:]
    empty_map = (
        jnp.full((heads_here, tokens_here), NEG_FILL, jnp.float32),
        jnp.zeros((heads_here, tokens_here), jnp.float32),
        jnp.zeros((heads_here, tokens_here, value_width), jnp.float32),
    )
    folded = (empty_map, empty_map)
    key_piece = lax.all_gather(key_rows, "sp", axis=0, tiled=True)
    value_piece = lax.all_gather(value_rows, "sp", axis=0, tiled=True)
    key_count = key_piece.shape[0]
    key_width = math.gcd(key_count, 1024)
    blocks = key_count // key_width
    key_blocks = key_piece.reshape(blocks, key_width, heads_here, 2 * QK)
    value_blocks = value_piece.reshape(blocks, key_width, heads_here, value_width)

    def advance(running, inputs):
        block_index, key_block, value_block = inputs
        key_start = block_index * key_width

        def compute(current):
            key_span = (key_start + jnp.arange(key_width, dtype=jnp.int32)) // SPAN
            visible = key_span[None, :] <= query_span[:, None]
            first = update_map(current[0], first_query, key_block[..., :QK], value_block, visible)
            second = update_map(current[1], second_query, key_block[..., QK:], value_block, visible)
            return (first, second)

        running = lax.cond(
            key_start < query_start + tokens_here, compute, lambda current: current, running
        )
        return (running, None)

    folded, _ = lax.scan(
        advance, folded, (jnp.arange(blocks, dtype=jnp.int32), key_blocks, value_blocks)
    )
    first_map, second_map = folded
    mixture = (
        first_map[2] / first_map[1][..., None]
        - diff_scale[:, None, None] * second_map[2] / second_map[1][..., None]
    )
    scale_back = lax.rsqrt(jnp.mean(mixture * mixture, axis=-1, keepdims=True) + NORM_EPS)
    attended = (mixture * scale_back * head_gain * HEAD_KEEP).astype(jnp.bfloat16)
    column_width = out_weight.shape[1]
    head_weight = out_weight.reshape(-1, value_width, column_width)
    weight_slice = head_weight
    projected = jnp.einsum(
        "htv,hvd->td",
        lax.all_gather(attended, "tp", axis=0, tiled=True),
        weight_slice,
        preferred_element_type=jnp.float32,
    )
    after_mixer = (residual.astype(jnp.float32) + projected).astype(jnp.bfloat16)
    mixer_float = after_mixer.astype(jnp.float32)
    partial_value = jnp.sum(mixer_float * mixer_float, axis=-1)
    square_total = lax.psum(partial_value, "tp")
    gain_slice = lax.dynamic_slice_in_dim(
        norm_gain, lax.axis_index("tp") * column_width, column_width, 0
    )
    normed = (mixer_float * lax.rsqrt(square_total / D + NORM_EPS)[:, None] * gain_slice).astype(
        jnp.bfloat16
    )
    experts = lax.axis_size("sp")
    top_count = expert_ids.shape[1]
    capacity = -(-(2 * tokens_here * top_count // experts) // 16) * 16
    chosen = expert_ids.reshape(-1)
    onehot = (chosen[:, None] == jnp.arange(experts, dtype=jnp.int32)[None, :]).astype(jnp.int32)
    rank_in = jnp.sum(jnp.cumsum(onehot, axis=0) * onehot, axis=1) - 1
    slot_index = chosen * capacity + rank_in
    owner_row = (
        jnp.full((experts * capacity,), tokens_here, jnp.int32)
        .at[slot_index]
        .set(jnp.arange(tokens_here * top_count, dtype=jnp.int32) // top_count)
    )
    padded = jnp.concatenate([normed, jnp.zeros((1, normed.shape[1]), jnp.bfloat16)], axis=0)
    outgoing = padded[owner_row].reshape(experts, capacity, normed.shape[1])
    returned_rows = run_experts(outgoing, gate_weight[0], up_weight[0], down_weight[0])
    picked = returned_rows.reshape(experts * capacity, -1)[slot_index].astype(jnp.float32)
    picked = picked.reshape(tokens_here, top_count, -1)
    weights = jax.nn.softmax(route_logit, axis=-1)
    routed = jnp.sum(picked * weights[..., None], axis=1)
    return (mixer_float + routed).astype(jnp.bfloat16)


def solution(mesh):
    return jax.shard_map(
        local,
        mesh=mesh,
        in_specs=(
            P("sp", "tp"),
            P("sp", "tp", None),
            P("sp", "tp", None),
            P("sp", "tp", None),
            P("tp"),
            P(),
            P(None, "tp"),
            P(),
            P("sp", None, "tp"),
            P("sp", None, "tp"),
            P("sp", None, "tp"),
            P("sp", None),
            P("sp", None),
        ),
        out_specs=P("sp", "tp"),
        check_vma=False,
    )
```

```python
import functools
import math

import jax
import jax.numpy as jnp
from jax import lax
from jax.experimental import pallas as pl
from jax.experimental.pallas import tpu as pltpu
from jax.sharding import PartitionSpec as P

D = 2048
QK = 64
SPAN = 64


NORM_EPS = 1e-05
CLAMP_LIMIT = 7.0
SWISH_ALPHA = 1.702
HEAD_KEEP = 0.8
NEG_FILL = -1e30


def attend_kernel(
    sp_size,
    queries,
    own_block,
    diff_scale,
    head_gain,
    attended,
    blocks,
    peak,
    total,
    accum,
    local_sem,
    along_send,
    across_send,
    recv,
):
    me = lax.axis_index("sp")
    rank = lax.axis_index("tp")
    pairs = sp_size // 2
    pair = me // 2
    side = lax.rem(me, 2)
    other = me + 1 - 2 * side
    tokens = queries.shape[0]
    width = head_gain.shape[1]
    heads = queries.shape[1] // width

    def place(index):
        return {"sp": index, "tp": rank}

    load = pltpu.make_async_copy(own_block, blocks.at[me], local_sem)
    load.start()
    barrier = pltpu.get_barrier_semaphore()

    def greet(index):
        pl.semaphore_signal(
            barrier, inc=1, device_id=place(index), device_id_type=pl.DeviceIdType.MESH
        )

    greet(other)

    @pl.when(pair > 0)
    def _():
        greet(me - 2)

    @pl.when(pair < pairs - 1)
    def _():
        greet(me + 2)

    pl.semaphore_wait(barrier, 1 + jnp.minimum(pair, 1) + jnp.minimum(pairs - 1 - pair, 1))
    peak[...] = jnp.full(peak.shape, NEG_FILL, jnp.float32)
    total[...] = jnp.zeros(total.shape, jnp.float32)
    accum[...] = jnp.zeros(accum.shape, jnp.float32)
    load.wait()

    def hand_on(block, send, back, target):
        return pltpu.make_async_remote_copy(
            src_ref=blocks.at[block],
            dst_ref=blocks.at[block],
            send_sem=send.at[back],
            recv_sem=recv.at[block],
            device_id=place(target),
            device_id_type=pl.DeviceIdType.MESH,
        )

    def compute(block):
        row = me * tokens + lax.broadcasted_iota(jnp.int32, (tokens, tokens), 0)
        col = block * tokens + lax.broadcasted_iota(jnp.int32, (tokens, tokens), 1)
        visible = col // SPAN <= row // SPAN
        for head in range(heads):
            value = blocks[block, 1, :, head * width : (head + 1) * width]
            for half in range(2):
                start = head * width + half * QK
                scores = lax.dot_general(
                    queries[:, start : start + QK],
                    blocks[block, 0, :, start : start + QK],
                    (((1,), (1,)), ((), ())),
                    preferred_element_type=jnp.float32,
                ) * QK ** (-0.5)
                scores = jnp.where(visible, scores, NEG_FILL)
                index = head * 2 + half
                old = peak[index]
                new = jnp.maximum(old, jnp.max(scores, axis=-1, keepdims=True))
                weights = jnp.where(visible, jnp.exp(scores - new), 0.0)
                rescale = jnp.exp(old - new)
                peak[index] = new
                total[index] = total[index] * rescale + jnp.sum(weights, axis=-1, keepdims=True)
                accum[index] = accum[index] * rescale + jnp.dot(
                    weights.astype(jnp.bfloat16), value, preferred_element_type=jnp.float32
                )

    @pl.loop(0, pair + 2)
    def _(back):
        @pl.when(back <= pair)
        def _():
            block = me - 2 * back

            @pl.when(back > 0)
            def _():
                hand_on(block, across_send, back, other).wait_recv()

            @pl.when(pair < pairs - 1)
            def _():
                hand_on(block, along_send, back, me + 2).start()

            @pl.when((back > 0) | (side == 0))
            def _():
                hand_on(block, across_send, back, other).start()

        second = other - 2 * (back - 1)
        use_second = (back >= 2) | ((back == 1) & (side == 1))

        @pl.loop(0, 2)
        def _(which):
            @pl.when((which == 1) & use_second)
            def _():
                hand_on(second, across_send, 0, other).wait_recv()

            @pl.when(((which == 0) & (back <= pair)) | ((which == 1) & use_second))
            def _():
                compute(jnp.where(which == 0, me - 2 * back, second))

    for head in range(heads):
        first = accum[head * 2] / total[head * 2]
        later = accum[head * 2 + 1] / total[head * 2 + 1]
        mixture = first - diff_scale[head] * later
        scale_back = lax.rsqrt(jnp.mean(mixture * mixture, axis=-1, keepdims=True) + NORM_EPS)
        attended[:, head * width : (head + 1) * width] = (
            mixture * scale_back * head_gain[...] * HEAD_KEEP
        ).astype(jnp.bfloat16)

    @pl.loop(0, pair + 1)
    def _(back):
        block = me - 2 * back

        @pl.when(pair < pairs - 1)
        def _():
            hand_on(block, along_send, back, me + 2).wait_send()

        @pl.when((back > 0) | (side == 0))
        def _():
            hand_on(block, across_send, back, other).wait_send()


def run_attention(queries, key_rows, value_rows, diff_scale, head_gain):
    sp_size = lax.axis_size("sp")
    tokens, heads, width = value_rows.shape
    own_block = jnp.stack(
        [key_rows.reshape(tokens, heads * width), value_rows.reshape(tokens, heads * width)]
    )
    dma = pltpu.SemaphoreType.DMA
    vmem = pl.BlockSpec(memory_space=pltpu.VMEM)
    return pl.pallas_call(
        functools.partial(attend_kernel, sp_size),
        out_shape=jax.ShapeDtypeStruct((tokens, heads * width), jnp.bfloat16),
        in_specs=[
            vmem,
            pl.BlockSpec(memory_space=pl.ANY),
            pl.BlockSpec(memory_space=pltpu.SMEM),
            vmem,
        ],
        out_specs=vmem,
        scratch_shapes=[
            pltpu.VMEM((sp_size,) + own_block.shape, jnp.bfloat16),
            pltpu.VMEM((heads * 2, tokens, 1), jnp.float32),
            pltpu.VMEM((heads * 2, tokens, 1), jnp.float32),
            pltpu.VMEM((heads * 2, tokens, width), jnp.float32),
            dma(()),
            dma((sp_size,)),
            dma((sp_size,)),
            dma((sp_size,)),
        ],
        compiler_params=pltpu.CompilerParams(
            collective_id=1, has_side_effects=True, vmem_limit_bytes=32 * 1024 * 1024
        ),
    )(queries.reshape(tokens, heads * width), own_block, diff_scale, head_gain[None])


def expert_kernel(
    sp_size,
    tp_size,
    groups,
    outgoing,
    gate_hbm,
    up_hbm,
    down_hbm,
    returned,
    rows_in,
    hidden,
    result,
    gate,
    up,
    down,
    weight_sem,
    local_sem,
    disp_send,
    disp_recv,
    ret_send,
    ret_recv,
    row_send,
    row_recv,
    hid_send,
    hid_recv,
):
    me = lax.axis_index("sp")
    rank = lax.axis_index("tp")
    parity = lax.rem(rank, 2)
    sibling = rank + 1 - 2 * parity
    chips = tp_size // 2
    chip = rank // 2
    span = sp_size // groups
    cap = outgoing.shape[1]
    feats = outgoing.shape[2]
    units = gate.shape[1]
    columns = down.shape[1]

    weights = [
        pltpu.make_async_copy(src, dst, weight_sem.at[i])
        for i, (src, dst) in enumerate(((gate_hbm, gate), (up_hbm, up), (down_hbm, down)))
    ]
    for copy in weights:
        copy.start()

    def peer_rank(step):
        return lax.rem(chip + step, chips) * 2 + parity

    barrier = pltpu.get_barrier_semaphore()
    for step in range(1, sp_size):
        pl.semaphore_signal(
            barrier,
            inc=1,
            device_id={"sp": lax.rem(me + step, sp_size), "tp": rank},
            device_id_type=pl.DeviceIdType.MESH,
        )
    for step in range(1, chips):
        pl.semaphore_signal(
            barrier,
            inc=1,
            device_id={"sp": me, "tp": peer_rank(step)},
            device_id_type=pl.DeviceIdType.MESH,
        )
    pl.semaphore_signal(
        barrier,
        inc=1,
        device_id={"sp": me, "tp": sibling},
        device_id_type=pl.DeviceIdType.MESH,
    )
    pl.semaphore_wait(barrier, sp_size - 1 + chips)

    def slot(step):
        return rows_in.at[step // span, rank, pl.ds((step % span) * cap, cap)]

    def dispatch(step):
        expert = lax.rem(me + sp_size - step, sp_size)
        return pltpu.make_async_remote_copy(
            src_ref=outgoing.at[expert],
            dst_ref=slot(step),
            send_sem=disp_send.at[step],
            recv_sem=disp_recv.at[step],
            device_id={"sp": expert, "tp": rank},
            device_id_type=pl.DeviceIdType.MESH,
        )

    own_in = pltpu.make_async_copy(outgoing.at[me], slot(0), local_sem.at[0])
    own_in.start()
    for step in range(1, sp_size):
        dispatch(step).start()

    def piece(buffer, send, recv, group, owner, target, send_slot):
        return pltpu.make_async_remote_copy(
            src_ref=buffer.at[group, owner],
            dst_ref=buffer.at[group, owner],
            send_sem=send.at[group, send_slot],
            recv_sem=recv.at[group, owner],
            device_id={"sp": me, "tp": target},
            device_id_type=pl.DeviceIdType.MESH,
        )

    def spread(buffer, send, recv, group):
        for step in range(1, chips):
            target = peer_rank(step)
            piece(buffer, send, recv, group, rank, target, target).start()
        piece(buffer, send, recv, group, rank, sibling, sibling).start()

    def collect(buffer, send, recv, group):
        for step in range(1, chips):
            owner = peer_rank(step)
            forward = piece(buffer, send, recv, group, owner, sibling, owner + 1 - 2 * parity)
            forward.wait_recv()
            forward.start()
        for step in range(chips):
            owner = peer_rank(step) + 1 - 2 * parity
            piece(buffer, send, recv, group, owner, sibling, sibling).wait_recv()

    unit_tile = math.gcd(units, 256)
    column_tile = math.gcd(columns, 256)

    def spread_rows(group):
        for place in range(span):
            def arrived(place=place):
                step = group * span + place
                pltpu.make_async_remote_copy(
                    src_ref=outgoing.at[0],
                    dst_ref=rows_in.at[group, rank, pl.ds(place * cap, cap)],
                    send_sem=disp_send.at[step],
                    recv_sem=disp_recv.at[step],
                    device_id={"sp": me, "tp": sibling},
                    device_id_type=pl.DeviceIdType.MESH,
                ).wait_recv()

            if place == 0:
                @pl.when(group == 0)
                def _():
                    own_in.wait()

                pl.when(group > 0)(arrived)
            else:
                arrived()
        spread(rows_in, row_send, row_recv, group)

    def run_up(group):
        collect(rows_in, row_send, row_recv, group)

        @pl.when(group == 0)
        def _():
            weights[0].wait()
            weights[1].wait()

        @pl.loop(0, units // unit_tile)
        def _(tile):
            cols = pl.ds(pl.multiple_of(tile * unit_tile, unit_tile), unit_tile)
            pre_gate = 0.0
            pre_up = 0.0
            for part in range(tp_size):
                block = rows_in[group, part]
                depth = pl.ds(part * feats, feats)
                pre_gate += jnp.dot(block, gate[depth, cols], preferred_element_type=jnp.float32)
                pre_up += jnp.dot(block, up[depth, cols], preferred_element_type=jnp.float32)
            capped = jnp.minimum(pre_gate, CLAMP_LIMIT)
            linear = jnp.clip(pre_up, -CLAMP_LIMIT, CLAMP_LIMIT)
            value = capped * jax.nn.sigmoid(SWISH_ALPHA * capped) * (linear + 1.0)
            hidden[group, rank, :, cols] = value.astype(jnp.bfloat16)

        spread(hidden, hid_send, hid_recv, group)

    def give_back(step):
        source = lax.rem(me + step, sp_size)
        return pltpu.make_async_remote_copy(
            src_ref=result.at[step // span, pl.ds((step % span) * cap, cap)],
            dst_ref=returned.at[me],
            send_sem=ret_send.at[step],
            recv_sem=ret_recv.at[step],
            device_id={"sp": source, "tp": rank},
            device_id_type=pl.DeviceIdType.MESH,
        )

    own_out = pltpu.make_async_copy(result.at[0, pl.ds(0, cap)], returned.at[me], local_sem.at[1])

    def run_down(group):
        collect(hidden, hid_send, hid_recv, group)

        @pl.when(group == 0)
        def _():
            weights[2].wait()

        @pl.loop(0, columns // column_tile)
        def _(tile):
            cols = pl.ds(pl.multiple_of(tile * column_tile, column_tile), column_tile)
            total = 0.0
            for part in range(tp_size):
                total += jnp.dot(
                    hidden[group, part],
                    down[pl.ds(part * units, units), cols],
                    preferred_element_type=jnp.float32,
                )
            result[group, :, cols] = total.astype(jnp.bfloat16)

        for place in range(span):
            if place == 0:
                @pl.when(group == 0)
                def _():
                    own_out.start()

                @pl.when(group > 0)
                def _():
                    give_back(group * span).start()
            else:
                give_back(group * span + place).start()

    @pl.loop(0, groups + 2)
    def _(turn):
        @pl.when(turn < groups)
        def _():
            spread_rows(turn)

        @pl.when((turn >= 1) & (turn < groups + 1))
        def _():
            run_up(turn - 1)

        @pl.when(turn >= 2)
        def _():
            run_down(turn - 2)

    own_out.wait()
    for step in range(1, sp_size):
        dispatch(step).wait_send()
    for step in range(1, sp_size):
        back = give_back(step)
        back.wait_send()
        pltpu.make_async_remote_copy(
            src_ref=result.at[0, pl.ds(0, cap)],
            dst_ref=returned.at[lax.rem(me + sp_size - step, sp_size)],
            send_sem=ret_send.at[step],
            recv_sem=ret_recv.at[step],
            device_id={"sp": lax.rem(me + step, sp_size), "tp": rank},
            device_id_type=pl.DeviceIdType.MESH,
        ).wait_recv()

    @pl.loop(0, groups)
    def _(group):
        for buffer, send, recv in ((rows_in, row_send, row_recv), (hidden, hid_send, hid_recv)):
            for step in range(1, chips):
                target = peer_rank(step)
                piece(buffer, send, recv, group, rank, target, target).wait_send()
                other = target + 1 - 2 * parity
                piece(buffer, send, recv, group, target, sibling, other).wait_send()
            piece(buffer, send, recv, group, rank, sibling, sibling).wait_send()


def run_experts(outgoing, gate_weight, up_weight, down_weight):
    sp_size, cap, feats = outgoing.shape
    tp_size = lax.axis_size("tp")
    groups = math.gcd(sp_size, 4)
    rows = sp_size // groups * cap
    units = gate_weight.shape[1]
    columns = down_weight.shape[1]
    dma = pltpu.SemaphoreType.DMA
    return pl.pallas_call(
        functools.partial(expert_kernel, sp_size, tp_size, groups),
        out_shape=jax.ShapeDtypeStruct((sp_size, cap, columns), jnp.bfloat16),
        in_specs=[pl.BlockSpec(memory_space=pltpu.VMEM)]
        + [pl.BlockSpec(memory_space=pl.ANY)] * 3,
        out_specs=pl.BlockSpec(memory_space=pl.ANY),
        scratch_shapes=[
            pltpu.VMEM((groups, tp_size, rows, feats), jnp.bfloat16),
            pltpu.VMEM((groups, tp_size, rows, units), jnp.bfloat16),
            pltpu.VMEM((groups, rows, columns), jnp.bfloat16),
            pltpu.VMEM(gate_weight.shape, jnp.bfloat16),
            pltpu.VMEM(up_weight.shape, jnp.bfloat16),
            pltpu.VMEM(down_weight.shape, jnp.bfloat16),
            dma((3,)),
            dma((2,)),
            dma((sp_size,)),
            dma((sp_size,)),
            dma((sp_size,)),
            dma((sp_size,)),
            dma((groups, tp_size)),
            dma((groups, tp_size)),
            dma((groups, tp_size)),
            dma((groups, tp_size)),
        ],
        compiler_params=pltpu.CompilerParams(
            collective_id=0, has_side_effects=True, vmem_limit_bytes=48 * 1024 * 1024
        ),
    )(outgoing, gate_weight, up_weight, down_weight)


def local(
    residual,
    queries,
    key_rows,
    value_rows,
    diff_scale,
    head_gain,
    out_weight,
    norm_gain,
    gate_weight,
    up_weight,
    down_weight,
    expert_ids,
    route_logit,
):
    tokens_here = queries.shape[0]
    attended = run_attention(queries, key_rows, value_rows, diff_scale, head_gain)
    column_width = out_weight.shape[1]
    gathered = lax.all_gather(attended, "tp", axis=0)
    projected = jnp.einsum(
        "rtv,rvd->td",
        gathered,
        out_weight.reshape(gathered.shape[0], -1, column_width),
        preferred_element_type=jnp.float32,
    )
    after_mixer = (residual.astype(jnp.float32) + projected).astype(jnp.bfloat16)
    mixer_float = after_mixer.astype(jnp.float32)
    partial_value = jnp.sum(mixer_float * mixer_float, axis=-1)
    square_total = lax.psum(partial_value, "tp")
    gain_slice = lax.dynamic_slice_in_dim(
        norm_gain, lax.axis_index("tp") * column_width, column_width, 0
    )
    normed = (mixer_float * lax.rsqrt(square_total / D + NORM_EPS)[:, None] * gain_slice).astype(
        jnp.bfloat16
    )
    experts = lax.axis_size("sp")
    top_count = expert_ids.shape[1]
    capacity = -(-(2 * tokens_here * top_count // experts) // 16) * 16
    chosen = expert_ids.reshape(-1)
    order = jnp.arange(chosen.shape[0], dtype=jnp.int32)
    earlier = (chosen[:, None] == chosen[None, :]) & (order[None, :] < order[:, None])
    rank_in = jnp.sum(earlier.astype(jnp.int32), axis=1)
    slot_index = (chosen * capacity + rank_in).reshape(tokens_here, top_count)
    slots = jnp.arange(experts * capacity, dtype=jnp.int32)
    holds = [slot_index[:, k][:, None] == slots[None, :] for k in range(top_count)]
    holds_any = functools.reduce(jnp.logical_or, holds)
    outgoing = (
        jnp.einsum(
            "ts,td->sd",
            holds_any.astype(jnp.bfloat16),
            normed,
            preferred_element_type=jnp.float32,
        )
        .astype(jnp.bfloat16)
        .reshape(experts, capacity, normed.shape[1])
    )
    returned_rows = run_experts(outgoing, gate_weight[0], up_weight[0], down_weight[0])
    flat_rows = returned_rows.reshape(experts * capacity, -1)
    weights = jax.nn.softmax(route_logit, axis=-1)
    routed = 0.0
    for k in range(top_count):
        picked = jnp.dot(
            holds[k].astype(jnp.bfloat16), flat_rows, preferred_element_type=jnp.float32
        )
        routed = routed + picked * weights[:, k : k + 1]
    return (mixer_float + routed).astype(jnp.bfloat16)


def solution(mesh):
    return jax.shard_map(
        local,
        mesh=mesh,
        in_specs=(
            P("sp", "tp"),
            P("sp", "tp", None),
            P("sp", "tp", None),
            P("sp", "tp", None),
            P("tp"),
            P(),
            P(None, "tp"),
            P(),
            P("sp", None, "tp"),
            P("sp", None, "tp"),
            P("sp", None, "tp"),
            P("sp", None),
            P("sp", None),
        ),
        out_specs=P("sp", "tp"),
        check_vma=False,
    )
```
